32 devices in a mesh: sp: 8 (over z, y), tp: 4 (over x, core).
Axes of the slice: x: 2, y: 2, z: 4, core: 2. Of those that a mesh axis runs over, the one named last changes fastest.
Arguments:
- queries: bfloat16 [2304, 2048], P('sp', 'tp'), as said below
- key_vectors: bfloat16 [2304, 2048], P('sp', 'tp'), as said below
- latents: bfloat16 [2304, 2048], P('sp'), as said below
- value_weight: bfloat16 [2048, 2048], P(None, 'tp'), as said below
- log_sums: float32 [2304, 32], P('sp', 'tp'), as said below
- out_first: bfloat16 [2304, 2048], P('sp', 'tp'), as said below
- out_second: bfloat16 [2304, 2048], P('sp', 'tp'), as said below
- cotangent: bfloat16 [2304, 2048], P('sp', 'tp'), may hold values from -6 to 6
- head_lambda: float32 [16], P('tp'), may hold values from 0.3 to 0.8
Outputs:
- grad_queries: float32 [2304, 2048], P('sp', 'tp')
- grad_keys: float32 [2304, 2048], P('sp', 'tp')
- grad_latents: bfloat16 [2304, 2048], P('sp', 'tp')
- grad_weight: float32 [2048, 2048], P('sp', 'tp')
The draws below stay inside these ranges and needn't reach their ends.
Inputs may be any that keep to these rules, and one draw needn't show every extreme that they name: queries with entries of standard deviation 1.75. `key_vectors`: keys with entries of standard deviation 1. `latents`: inputs of standard deviation 1. `value_weight`: weights scaled by the inverse square root of 2048. `log_sums`: each row's log-sum of exponentials of its causal scores, for the given queries and keys. `out_first`: the first map's attention output for the given queries, keys, values and log-sums. `out_second`: the second map's attention output, likewise.
All inputs are finite; a program needn't handle non-finite values.
Results may differ from the reference program's by a relative error of at most 0.022.
Values may be sent and summed in bfloat16 or wider, within the bound.
A program may use at most 192 MiB of HBM per device.

```python
import jax
import jax.numpy as jnp
from jax import lax

D = 2048
HEADS = 16
DH = 64
DV = 128
TOK_DEV = 288
TOKENS = 2304
N_SP = 8
N_TP = 4


def build_inputs(key):
    queries = (1.75 * jax.random.normal(jax.random.fold_in(key, 101), (TOKENS, HEADS * 2 * DH), jnp.float32)).astype(jnp.bfloat16)
    key_vectors = jax.random.normal(jax.random.fold_in(key, 102), (TOKENS, HEADS * 2 * DH), jnp.float32).astype(jnp.bfloat16)
    latents = jax.random.normal(jax.random.fold_in(key, 103), (TOKENS, D), jnp.float32).astype(jnp.bfloat16)
    value_weight = (jax.random.normal(jax.random.fold_in(key, 104), (D, HEADS * DV), jnp.float32) * D ** (-0.5)).astype(jnp.bfloat16)
    values = jnp.dot(latents, value_weight, preferred_element_type=jnp.float32).astype(jnp.bfloat16)
    blocks = TOKENS // TOK_DEV
    query_heads = queries.astype(jnp.float32).reshape(blocks, TOK_DEV, HEADS, 2, DH)
    key_heads = key_vectors.astype(jnp.float32).reshape(TOKENS, HEADS, 2, DH)
    value_heads = values.astype(jnp.float32).reshape(TOKENS, HEADS, DV)
    positions = jnp.arange(TOKENS, dtype=jnp.int32)

    def one_block(pair):
        block_rows, block_index = pair
        query_pos = block_index * TOK_DEV + jnp.arange(TOK_DEV, dtype=jnp.int32)
        scores = jnp.einsum('nhad,mhad->hanm', block_rows, key_heads) * DH ** (-0.5)
        causal = query_pos[:, None] >= positions[None, :]
        scores = jnp.where(causal, scores, -1e+30)
        highest = jnp.max(scores, axis=-1, keepdims=True)
        expo = jnp.exp(scores - highest)
        total = jnp.sum(expo, axis=-1, keepdims=True)
        outputs = jnp.einsum('hanm,mhe->nhae', expo / total, value_heads)
        sums = (highest + jnp.log(total))[..., 0].transpose(2, 0, 1)
        return (sums, outputs)
    sums, outputs = lax.map(one_block, (query_heads, jnp.arange(blocks, dtype=jnp.int32)))
    log_sums = sums.reshape(TOKENS, HEADS * 2)
    out_first = outputs[:, :, :, 0, :].reshape(TOKENS, HEADS * DV).astype(jnp.bfloat16)
    out_second = outputs[:, :, :, 1, :].reshape(TOKENS, HEADS * DV).astype(jnp.bfloat16)
    return (queries, key_vectors, latents, value_weight, log_sums, out_first, out_second)


def draw_queries(key, part):
    return build_inputs(key)[0]


def draw_key_vectors(key, part):
    return build_inputs(key)[1]


def draw_latents(key, part):
    return build_inputs(key)[2]


def draw_value_weight(key, part):
    return build_inputs(key)[3]


def draw_log_sums(key, part):
    return build_inputs(key)[4]


def draw_out_first(key, part):
    return build_inputs(key)[5]


def draw_out_second(key, part):
    return build_inputs(key)[6]


def strengthened(entries, key, source, target, shards_of, factor):
    def block_of(dim):
        return (jnp.arange(entries.shape[dim]) // (entries.shape[dim] // shards_of)).reshape((-1,) + (1,) * (entries.ndim - 1 - dim))

    one_side = jax.random.permutation(key, shards_of)[block_of(target)]
    far = (block_of(target) + shards_of // 2) % shards_of
    return jnp.where((block_of(source) == one_side) | (block_of(source) == far), factor * entries, entries)


def block_scale(key, extent, shards, least, largest):
    factor_of = 1.0
    for dim, blocks in shards:
        steps = jax.random.uniform(jax.random.fold_in(jax.random.fold_in(key, 6), dim), (blocks,), jnp.float32, least / len(shards), largest / len(shards))
        factor_of = factor_of * jnp.repeat(jnp.exp(steps), extent[dim] // blocks).reshape((-1,) + (1,) * (len(extent) - 1 - dim))
    return factor_of


def noise_with(own_key, extent, spread, limit, cuts, heavy, kind=jnp.bfloat16):
    result = spread * jax.random.normal(own_key, extent, jnp.float32)
    if cuts:
        result = result * block_scale(own_key, extent, cuts, -0.22, 0.18)
    return jnp.clip(strengthened(result, jax.random.fold_in(own_key, 3), *heavy), -limit, limit).astype(kind)


def setup_inputs(seed: int = 0) -> dict:
    arg_keys = jax.random.split(jax.random.key(seed), 10)
    return {
        "queries": draw_queries(jax.random.fold_in(arg_keys[9], 71), 0),
        "key_vectors": draw_key_vectors(jax.random.fold_in(arg_keys[9], 71), 0),
        "latents": draw_latents(jax.random.fold_in(arg_keys[9], 71), 0),
        "value_weight": draw_value_weight(jax.random.fold_in(arg_keys[9], 71), 0),
        "log_sums": draw_log_sums(jax.random.fold_in(arg_keys[9], 71), 0),
        "out_first": draw_out_first(jax.random.fold_in(arg_keys[9], 71), 0),
        "out_second": draw_out_second(jax.random.fold_in(arg_keys[9], 71), 0),
        "cotangent": noise_with(arg_keys[7], (TOKENS, HEADS * DV), 1.0, 6.0, ((0, 8), (1, 4)), (0, 1, 8, 2.0)),
        "head_lambda": jnp.clip(0.3 + 0.5 * jax.random.uniform(arg_keys[8], (HEADS,), jnp.float32) ** block_scale(arg_keys[8], (HEADS,), ((0, 4),), -0.2, 0.2), 0.3, 0.8),
    }


def row_terms(out_first, out_second, cotangent, head_lambda):
    count = out_first.shape[0]
    head_count = head_lambda.shape[0]
    first = out_first.astype(jnp.float32).reshape(count, head_count, DV)
    second = out_second.astype(jnp.float32).reshape(count, head_count, DV)
    mixed = first - head_lambda[None, :, None] * second
    inverse = lax.rsqrt(lax.optimization_barrier(jnp.mean(mixed * mixed, axis=-1, keepdims=True)) + 1e-06)
    normed = mixed * inverse
    grad_out = cotangent.astype(jnp.float32).reshape(count, head_count, DV)
    grad_mixed = inverse * (grad_out - normed * lax.optimization_barrier(jnp.mean(grad_out * normed, axis=-1, keepdims=True)))
    grad_rows = grad_mixed.astype(jnp.bfloat16)
    widened = lax.optimization_barrier(grad_rows).astype(jnp.float32)
    row_dots = jnp.stack([lax.optimization_barrier(jnp.sum(widened * first, axis=-1)), lax.optimization_barrier(jnp.sum(widened * second, axis=-1))], axis=-1)
    return (grad_rows.reshape(count, head_count * DV), row_dots.reshape(count, head_count * 2))

def block_grads(query_rows, grad_rows, lse_rows, dot_rows, query_pos, key_rows, value_rows, key_pos, head_lambda):
    count = query_rows.shape[0]
    width = key_rows.shape[0]
    head_count = head_lambda.shape[0]
    score_scale = DH ** (-0.5)
    query_heads = query_rows.astype(jnp.float32).reshape(count, head_count, 2, DH)
    key_heads = key_rows.astype(jnp.float32).reshape(width, head_count, 2, DH)
    grad_heads = grad_rows.astype(jnp.float32).reshape(count, head_count, DV)
    value_heads = value_rows.astype(jnp.float32).reshape(width, head_count, DV)
    scores = jnp.einsum('nhad,mhad->hanm', query_heads, key_heads) * score_scale
    causal = query_pos[:, None] >= key_pos[None, :]
    shifts = lse_rows.reshape(count, head_count, 2).transpose(1, 2, 0)[..., None]
    probs = jnp.exp(jnp.where(causal, scores - shifts, -1e+30))
    d_attn = jnp.einsum('nhe,mhe->hnm', grad_heads, value_heads)
    dots = dot_rows.reshape(count, head_count, 2).transpose(1, 2, 0)[..., None]
    map_weight = jnp.stack([jnp.ones_like(head_lambda), -head_lambda], axis=1)[:, :, None, None]
    d_scores = (map_weight * probs * (d_attn[:, None] - dots)).astype(jnp.bfloat16)
    d_scores = lax.optimization_barrier(d_scores).astype(jnp.float32)
    weights = (probs[:, 0] - head_lambda[:, None, None] * probs[:, 1]).astype(jnp.bfloat16)
    weights = lax.optimization_barrier(weights).astype(jnp.float32)
    grad_q = jnp.einsum('hanm,mhad->nhad', d_scores, key_heads) * score_scale
    grad_k = jnp.einsum('hanm,nhad->mhad', d_scores, query_heads) * score_scale
    grad_v = jnp.einsum('hnm,nhe->mhe', weights, grad_heads)
    return (grad_q.reshape(count, -1), grad_k.reshape(width, -1), grad_v.reshape(width, -1))

def reference(queries, key_vectors, latents, value_weight, log_sums, out_first, out_second, cotangent, head_lambda):
    values = jnp.dot(latents, value_weight, preferred_element_type=jnp.float32).astype(jnp.bfloat16)
    grad_rows, row_dots = row_terms(out_first, out_second, cotangent, head_lambda)
    positions = jnp.arange(TOKENS, dtype=jnp.int32)

    def per_head(index):
        query_head = lax.dynamic_slice_in_dim(queries, index * 2 * DH, 2 * DH, 1)
        key_head = lax.dynamic_slice_in_dim(key_vectors, index * 2 * DH, 2 * DH, 1)
        value_head = lax.dynamic_slice_in_dim(values, index * DV, DV, 1)
        grad_head = lax.dynamic_slice_in_dim(grad_rows, index * DV, DV, 1)
        lse_head = lax.dynamic_slice_in_dim(log_sums, index * 2, 2, 1)
        dot_head = lax.dynamic_slice_in_dim(row_dots, index * 2, 2, 1)
        lambda_one = lax.dynamic_slice_in_dim(head_lambda, index, 1, 0)

        def block_step(totals, block_index):
            first_row = (block_index * TOK_DEV).astype(jnp.int32)
            query_pos = first_row + jnp.arange(TOK_DEV, dtype=jnp.int32)
            grad_q, grad_k, grad_v = block_grads(lax.dynamic_slice_in_dim(query_head, first_row, TOK_DEV, 0), lax.dynamic_slice_in_dim(grad_head, first_row, TOK_DEV, 0), lax.dynamic_slice_in_dim(lse_head, first_row, TOK_DEV, 0), lax.dynamic_slice_in_dim(dot_head, first_row, TOK_DEV, 0), query_pos, key_head, value_head, positions, lambda_one)
            return ((totals[0] + grad_k, totals[1] + grad_v), grad_q)
        initial = (jnp.zeros((TOKENS, 2 * DH), jnp.float32), jnp.zeros((TOKENS, DV), jnp.float32))
        totals, grad_blocks = lax.scan(block_step, initial, jnp.arange(N_SP, dtype=jnp.int32))
        return (grad_blocks.reshape(TOKENS, 2 * DH), totals[0], totals[1])
    grad_q, grad_k, grad_v = lax.map(per_head, jnp.arange(HEADS, dtype=jnp.int32))
    grad_queries = grad_q.transpose(1, 0, 2).reshape(TOKENS, HEADS * 2 * DH)
    grad_keys = grad_k.transpose(1, 0, 2).reshape(TOKENS, HEADS * 2 * DH)
    grad_values = grad_v.transpose(1, 0, 2).reshape(TOKENS, HEADS * DV).astype(jnp.bfloat16)
    grad_weight = lax.dot_general(latents, grad_values, (((0,), (0,)), ((), ())), preferred_element_type=jnp.float32)
    value_groups = grad_values.reshape(TOKENS, N_TP, -1).transpose(1, 0, 2)
    weight_groups = value_weight.reshape(D, N_TP, -1).transpose(1, 0, 2)

    def add_group(total, pair):
        partial_sum = lax.dot_general(pair[0], pair[1], (((1,), (1,)), ((), ())), preferred_element_type=jnp.float32)
        rounded = lax.optimization_barrier(partial_sum.astype(jnp.bfloat16))
        return (total + rounded.astype(jnp.float32), None)
    latent_total, unused = lax.scan(add_group, jnp.zeros((TOKENS, D), jnp.float32), (value_groups, weight_groups))
    return (grad_queries, grad_keys, latent_total.astype(jnp.bfloat16), grad_weight)
```

```python
import functools

import jax
import jax.numpy as jnp
from jax import lax
from jax.experimental import pallas as pl
from jax.experimental.pallas import tpu as pltpu
from jax.sharding import PartitionSpec as P

DH = 64
DV = 128
BLOCK = 256


def row_terms(out_first, out_second, cotangent, head_lambda):
    count = out_first.shape[0]
    head_count = head_lambda.shape[0]
    first = out_first.astype(jnp.float32).reshape(count, head_count, DV)
    second = out_second.astype(jnp.float32).reshape(count, head_count, DV)
    mixed = first - head_lambda[None, :, None] * second
    inverse = lax.rsqrt(jnp.mean(mixed * mixed, axis=-1, keepdims=True) + 1e-06)
    normed = mixed * inverse
    grad_out = cotangent.astype(jnp.float32).reshape(count, head_count, DV)
    grad_mixed = inverse * (grad_out - normed * jnp.mean(grad_out * normed, axis=-1, keepdims=True))
    grad_rows = grad_mixed.astype(jnp.bfloat16)
    widened = lax.optimization_barrier(grad_rows).astype(jnp.float32)
    row_dots = jnp.stack(
        [jnp.sum(widened * first, axis=-1), jnp.sum(widened * second, axis=-1)], axis=-1
    )
    return (grad_rows.reshape(count, head_count * DV), row_dots.reshape(count, head_count * 2))


def block_grads(
    query_rows, grad_rows, lse_rows, dot_rows, query_pos, key_rows, value_rows, key_pos, head_lambda
):
    count = query_rows.shape[0]
    width = key_rows.shape[0]
    head_count = head_lambda.shape[0]
    score_scale = DH ** (-0.5)
    query_heads = query_rows.reshape(count, head_count, 2, DH)
    key_heads = key_rows.reshape(width, head_count, 2, DH)
    grad_heads = grad_rows.reshape(count, head_count, DV)
    value_heads = value_rows.reshape(width, head_count, DV)
    scores = (
        jnp.einsum("nhad,mhad->hanm", query_heads, key_heads, preferred_element_type=jnp.float32)
        * score_scale
    )
    causal = query_pos[:, None] >= key_pos[None, :]
    shifts = lse_rows.reshape(count, head_count, 2).transpose(1, 2, 0)[..., None]
    probs = jnp.exp(jnp.where(causal, scores - shifts, -1e30))
    d_attn = jnp.einsum("nhe,mhe->hnm", grad_heads, value_heads, preferred_element_type=jnp.float32)
    dots = dot_rows.reshape(count, head_count, 2).transpose(1, 2, 0)[..., None]
    map_weight = jnp.stack([jnp.ones_like(head_lambda), -head_lambda], axis=1)[:, :, None, None]
    d_scores = (map_weight * probs * (d_attn[:, None] - dots)).astype(jnp.bfloat16)
    weights = (probs[:, 0] - head_lambda[:, None, None] * probs[:, 1]).astype(jnp.bfloat16)
    grad_q = (
        jnp.einsum("hanm,mhad->nhad", d_scores, key_heads, preferred_element_type=jnp.float32)
        * score_scale
    )
    grad_k = (
        jnp.einsum("hanm,nhad->mhad", d_scores, query_heads, preferred_element_type=jnp.float32)
        * score_scale
    )
    grad_v = jnp.einsum("hnm,nhe->mhe", weights, grad_heads, preferred_element_type=jnp.float32)
    return (grad_q.reshape(count, -1), grad_k.reshape(width, -1), grad_v.reshape(width, -1))


def per_device(
    queries,
    key_vectors,
    latents,
    value_weight,
    log_sums,
    out_first,
    out_second,
    cotangent,
    head_lambda,
):
    local_rows = queries.shape[0]
    offset = lax.axis_index("sp") * local_rows
    positions = offset + jnp.arange(local_rows, dtype=jnp.int32)
    last_row = offset + local_rows - 1
    values = jnp.dot(latents, value_weight, preferred_element_type=jnp.float32).astype(jnp.bfloat16)
    grad_rows, row_dots = row_terms(out_first, out_second, cotangent, head_lambda)
    gathered_stats = (
        lax.all_gather(log_sums, "sp", axis=0, tiled=True),
        lax.all_gather(row_dots, "sp", axis=0, tiled=True),
    )
    key_rows = lax.all_gather(key_vectors, "sp", axis=0, tiled=True)
    value_rows = lax.all_gather(values, "sp", axis=0, tiled=True)
    count = key_rows.shape[0]

    def compute(current):
        key_pos = jnp.arange(count, dtype=jnp.int32)
        grad_q, unused_k, unused_v = block_grads(
            queries,
            grad_rows,
            log_sums,
            row_dots,
            positions,
            key_rows,
            value_rows,
            key_pos,
            head_lambda,
        )
        return grad_q

    grad_queries = lax.cond(
        jnp.int32(0) <= last_row,
        compute,
        lambda current: current,
        jnp.zeros((local_rows, queries.shape[1]), jnp.float32),
    )
    start_totals = (
        jnp.zeros((local_rows, key_vectors.shape[1]), jnp.float32),
        jnp.zeros((local_rows, values.shape[1]), jnp.float32),
    )
    query_rows = lax.all_gather(queries, "sp", axis=0, tiled=True)
    grad_piece = lax.all_gather(grad_rows, "sp", axis=0, tiled=True)
    add_count = query_rows.shape[0]

    def compute(current):
        query_pos = jnp.arange(add_count, dtype=jnp.int32)
        lse_rows = gathered_stats[0]
        dot_rows = gathered_stats[1]
        unused_q, grad_k, grad_v = block_grads(
            query_rows,
            grad_piece,
            lse_rows,
            dot_rows,
            query_pos,
            key_vectors,
            values,
            positions,
            head_lambda,
        )
        return (grad_k, grad_v)

    grad_keys, grad_values = lax.cond(
        jnp.int32(0) + add_count - 1 >= offset, compute, lambda current: current, start_totals
    )
    values_grad = grad_values.astype(jnp.bfloat16)
    grad_weight = lax.psum_scatter(
        lax.dot_general(
            latents, values_grad, (((0,), (0,)), ((), ())), preferred_element_type=jnp.float32
        ).astype(jnp.bfloat16),
        "sp",
        scatter_dimension=0,
        tiled=True,
    ).astype(jnp.float32)
    latent_partial = lax.dot_general(
        values_grad, value_weight, (((1,), (1,)), ((), ())), preferred_element_type=jnp.float32
    )
    grad_latents = lax.psum_scatter(
        latent_partial.astype(jnp.bfloat16), "tp", scatter_dimension=1, tiled=True
    )
    return (grad_queries, grad_keys, grad_latents, grad_weight)


def exchange_kernel(axis, n, parts, *refs):
    swap_blocks(axis, n, refs[:parts], refs[parts : 2 * parts], *refs[2 * parts :])


def swap_blocks(axis, n, ins, outs, send_sem, recv_sem, local_sem, prepare=lambda: None):
    parts = len(ins)
    me = lax.axis_index(axis)
    barrier = pltpu.get_barrier_semaphore()
    for step in range(1, n):
        peer = lax.rem(me + step, n)
        pl.semaphore_signal(
            barrier, inc=1, device_id={axis: peer}, device_id_type=pl.DeviceIdType.MESH
        )
    prepare()
    pl.semaphore_wait(barrier, n - 1)

    def remote(part, step, slot):
        peer = lax.rem(me + step, n)
        return pltpu.make_async_remote_copy(
            src_ref=ins[part].at[peer],
            dst_ref=outs[part].at[slot],
            send_sem=send_sem.at[part, step],
            recv_sem=recv_sem.at[part, step],
            device_id={axis: peer},
            device_id_type=pl.DeviceIdType.MESH,
        )

    order = sorted(range(1, n), key=lambda step: -min(step, n - step))
    for part in reversed(range(parts)):
        for step in order:
            remote(part, step, me).start()
    for part in range(parts):
        own = pltpu.make_async_copy(ins[part].at[me], outs[part].at[me], local_sem.at[part])
        own.start()
        own.wait()
    for part in range(parts):
        for step in order:
            remote(part, step, lax.rem(me + n - step, n)).wait_recv()
    for part in range(parts):
        for step in order:
            remote(part, step, me).wait_send()


def exchange(arrays, axis, n, collective_id):
    parts = len(arrays)
    sent = sum(a.size * a.dtype.itemsize for a in arrays)
    return pl.pallas_call(
        functools.partial(exchange_kernel, axis, n, parts),
        out_shape=[jax.ShapeDtypeStruct(a.shape, a.dtype) for a in arrays],
        in_specs=[pl.BlockSpec(memory_space=pltpu.VMEM)] * parts,
        out_specs=[pl.BlockSpec(memory_space=pltpu.VMEM)] * parts,
        scratch_shapes=[
            pltpu.SemaphoreType.DMA((parts, n)),
            pltpu.SemaphoreType.DMA((parts, n)),
            pltpu.SemaphoreType.DMA((parts,)),
        ],
        compiler_params=pltpu.CompilerParams(collective_id=collective_id, has_side_effects=True),
        cost_estimate=pl.CostEstimate(flops=0, bytes_accessed=sent * 16, transcendentals=0),
    )(*arrays)


def head_of(index):
    return slice(index * DV, (index + 1) * DV)


def send_kernel(
    axis, n, q_ref, k_ref, v_ref, first_ref, second_ref, cot_ref, lse_ref, lambda_ref,
    x_out, stats_out, x_s, stats_s, *sems
):
    def prepare():
        score_scale = jnp.bfloat16(DH**-0.5)
        columns = []
        stats_s[...] = jnp.zeros_like(stats_s)
        for head in range(n // 2):
            lanes = head_of(head)
            first = first_ref[:, lanes].astype(jnp.float32)
            second = second_ref[:, lanes].astype(jnp.float32)
            mixed = first - lambda_ref[head] * second
            inverse = lax.rsqrt(jnp.mean(mixed * mixed, axis=-1, keepdims=True) + 1e-06)
            normed = mixed * inverse
            grad_out = cot_ref[:, lanes].astype(jnp.float32)
            mean_dot = jnp.mean(grad_out * normed, axis=-1, keepdims=True)
            grad_rows = (inverse * (grad_out - normed * mean_dot)).astype(jnp.bfloat16)
            widened = grad_rows.astype(jnp.float32)
            columns.append(jnp.sum(widened * first, axis=-1, keepdims=True))
            columns.append(jnp.sum(widened * second, axis=-1, keepdims=True))
            q_pair = q_ref[:, lanes] * score_scale
            k_pair = k_ref[:, lanes]
            for m in range(2):
                unit = 2 * head + m
                half = slice(m * DH, (m + 1) * DH)
                x_s[unit, :, 0 : 2 * DH] = jnp.concatenate(
                    [q_pair[:, half], k_pair[:, half]], axis=1
                )
                x_s[unit, :, 2 * DH : 2 * DH + DV] = v_ref[:, lanes]
                x_s[unit, :, 2 * DH + DV :] = grad_rows
        dots = jnp.concatenate(columns, axis=1).T
        for unit in range(n):
            stats_s[unit, 0:1, :] = lse_ref[unit : unit + 1, :]
            stats_s[unit, 1:2, :] = dots[unit : unit + 1, :]

    swap_blocks(axis, n, (x_s, stats_s), (x_out, stats_out), *sems, prepare=prepare)


def send_units(queries, keys, values, first, second, cotangent, lse, head_lambda, n):
    rows = queries.shape[0]
    shapes = [((n, rows, 2 * DH + 2 * DV), jnp.bfloat16), ((n, 8, rows), jnp.float32)]
    vmem = pl.BlockSpec(memory_space=pltpu.VMEM)
    return pl.pallas_call(
        functools.partial(send_kernel, "sp", n),
        out_shape=[jax.ShapeDtypeStruct(*shape) for shape in shapes],
        in_specs=[vmem] * 7 + [pl.BlockSpec(memory_space=pltpu.SMEM)],
        out_specs=[vmem] * 2,
        scratch_shapes=[pltpu.VMEM(*shape) for shape in shapes]
        + [
            pltpu.SemaphoreType.DMA((2, n)),
            pltpu.SemaphoreType.DMA((2, n)),
            pltpu.SemaphoreType.DMA((2,)),
        ],
        compiler_params=pltpu.CompilerParams(collective_id=1, has_side_effects=True),
        cost_estimate=pl.CostEstimate(
            flops=0, bytes_accessed=queries.size * 64, transcendentals=0
        ),
    )(queries, keys, values, first, second, cotangent, lse, head_lambda)


def unpack_kernel(x_ref, lambda_ref, q_ref, k_ref, v_ref):
    for head in range(x_ref.shape[0] // 2):
        lanes = head_of(head)
        weight = -lambda_ref[head]
        first = x_ref[2 * head].astype(jnp.float32)
        second = x_ref[2 * head + 1].astype(jnp.float32) * weight
        q_ref[:, lanes] = jnp.concatenate([first[:, :DH], second[:, :DH]], axis=1) * DH ** (-0.5)
        k_ref[:, lanes] = jnp.concatenate(
            [first[:, DH : 2 * DH], second[:, DH : 2 * DH]], axis=1
        )
        v_ref[:, lanes] = (first[:, 2 * DH :] + second[:, 2 * DH :]).astype(jnp.bfloat16)


def unpack(grads, head_lambda):
    n, rows, _ = grads.shape
    vmem = pl.BlockSpec(memory_space=pltpu.VMEM)
    kinds = (jnp.float32, jnp.float32, jnp.bfloat16)
    return pl.pallas_call(
        unpack_kernel,
        out_shape=[jax.ShapeDtypeStruct((rows, n * DH), kind) for kind in kinds],
        in_specs=[vmem, pl.BlockSpec(memory_space=pltpu.SMEM)],
        out_specs=[vmem] * 3,
        cost_estimate=pl.CostEstimate(flops=0, bytes_accessed=grads.size * 6, transcendentals=0),
    )(grads, head_lambda)


def attention_kernel(block, x_ref, stats_ref, o_ref, q_s, k_s, kt_s, dqt_s, dk_s, dv_s):
    blocks = x_ref.shape[0] // block

    def rows_of(index):
        return pl.ds(pl.multiple_of(index * block, block), block)

    def prologue(index, carry):
        rows = rows_of(index)
        pair = x_ref[rows, 0 : 2 * DH]
        q_s[rows, :] = pair[:, :DH]
        keys = pair[:, DH:]
        k_s[rows, :] = keys
        kt_s[index] = keys.T
        dqt_s[index] = jnp.zeros((DH, block), jnp.float32)
        return carry

    lax.fori_loop(0, blocks, prologue, 0)

    def tile(key_index, query_index, diagonal):
        key_rows, query_rows = rows_of(key_index), rows_of(query_index)
        queries = q_s[query_rows, :]
        grads = x_ref[query_rows, 2 * DH + DV :]
        nt = (((1,), (1,)), ((), ()))
        scores = lax.dot_general(
            k_s[key_rows, :], queries, nt, preferred_element_type=jnp.float32
        )
        stats = stats_ref[query_index]
        shifted = scores - stats[0:1, :]
        if diagonal:
            key_at = lax.broadcasted_iota(jnp.int32, (block, block), 0)
            query_at = lax.broadcasted_iota(jnp.int32, (block, block), 1)
            shifted = jnp.where(query_at >= key_at, shifted, -1e30)
        probs = jnp.exp(shifted)
        d_attn = lax.dot_general(
            x_ref[key_rows, 2 * DH : 2 * DH + DV], grads, nt, preferred_element_type=jnp.float32
        )
        d_scores = (probs * (d_attn - stats[1:2, :])).astype(jnp.bfloat16)
        weights = probs.astype(jnp.bfloat16)
        dk = jnp.dot(d_scores, queries, preferred_element_type=jnp.float32)
        dv = jnp.dot(weights, grads, preferred_element_type=jnp.float32)
        dqt_s[query_index] += jnp.dot(
            kt_s[key_index], d_scores, preferred_element_type=jnp.float32
        )
        if diagonal:
            dk_s[...] = dk
            dv_s[...] = dv
        else:
            dk_s[...] += dk
            dv_s[...] += dv

    def column(key_index, carry):
        tile(key_index, key_index, True)

        def inner(query_index, carry):
            tile(key_index, query_index, False)
            return carry

        lax.fori_loop(key_index + 1, blocks, inner, 0)
        out = [dqt_s[key_index].T, dk_s[...], dv_s[...]]
        o_ref[rows_of(key_index), :] = jnp.concatenate(out, axis=1).astype(jnp.bfloat16)
        return carry

    lax.fori_loop(0, blocks, column, 0)


def attention(x, stats, block):
    count = x.shape[0]
    pairs = count * (count + block) // 2
    return pl.pallas_call(
        functools.partial(attention_kernel, block),
        out_shape=jax.ShapeDtypeStruct((count, 2 * DH + DV), jnp.bfloat16),
        in_specs=[pl.BlockSpec(memory_space=pltpu.VMEM)] * 2,
        out_specs=pl.BlockSpec(memory_space=pltpu.VMEM),
        scratch_shapes=[
            pltpu.VMEM((count, DH), jnp.bfloat16),
            pltpu.VMEM((count, DH), jnp.bfloat16),
            pltpu.VMEM((count // block, DH, block), jnp.bfloat16),
            pltpu.VMEM((count // block, DH, block), jnp.float32),
            pltpu.VMEM((block, DH), jnp.float32),
            pltpu.VMEM((block, DV), jnp.float32),
        ],
        cost_estimate=pl.CostEstimate(
            flops=2 * pairs * 448, bytes_accessed=count * 1600, transcendentals=pairs
        ),
    )(x, stats)


def weight_kernel(
    axis, n, lat_ref, dv_ref, o_ref, to_pair, from_pair, sums, from_line,
    pair_send, pair_recv, line_send, line_recv
):
    line = n // 2
    me = lax.axis_index(axis)
    place, side = me // 2, lax.rem(me, 2)
    partner = 2 * place + 1 - side
    width = lat_ref.shape[1] // n
    mesh_id = pl.DeviceIdType.MESH

    def at(step):
        return lax.rem(place + step, line)

    def term(unit):
        columns = pl.ds(pl.multiple_of(unit * width, width), width)
        return lax.dot_general(
            lat_ref[:, columns],
            dv_ref[...],
            (((0,), (0,)), ((), ())),
            preferred_element_type=jnp.float32,
        )

    def pair_copy(step):
        return pltpu.make_async_remote_copy(
            src_ref=to_pair.at[step],
            dst_ref=from_pair.at[step],
            send_sem=pair_send.at[step],
            recv_sem=pair_recv.at[step],
            device_id={axis: partner},
            device_id_type=mesh_id,
        )

    def line_copy(step):
        return pltpu.make_async_remote_copy(
            src_ref=sums.at[step],
            dst_ref=from_line.at[step],
            send_sem=line_send.at[step],
            recv_sem=line_recv.at[step],
            device_id={axis: 2 * at(step) + side},
            device_id_type=mesh_id,
        )

    barrier = pltpu.get_barrier_semaphore()
    pl.semaphore_signal(barrier, inc=1, device_id={axis: partner}, device_id_type=mesh_id)
    for step in range(1, line):
        pl.semaphore_signal(
            barrier, inc=1, device_id={axis: 2 * at(step) + side}, device_id_type=mesh_id
        )
    order = sorted(range(1, line), key=lambda step: -min(step, line - step)) + [0]
    to_pair[order[0]] = term(2 * at(order[0]) + 1 - side).astype(jnp.bfloat16)
    pl.semaphore_wait(barrier, line)
    pair_copy(order[0]).start()
    for step in order[1:]:
        to_pair[step] = term(2 * at(step) + 1 - side).astype(jnp.bfloat16)
        pair_copy(step).start()
    for step in order:
        own = term(2 * at(step) + side)
        pair_copy(step).wait_recv()
        total = own + from_pair[step].astype(jnp.float32)
        if step == 0:
            o_ref[...] = total
        else:
            sums[step] = total.astype(jnp.bfloat16)
            line_copy(step).start()
    for step in order[:-1]:
        line_copy(step).wait_recv()
        o_ref[...] += from_line[step].astype(jnp.float32)
    for step in order:
        pair_copy(step).wait_send()
    for step in order[:-1]:
        line_copy(step).wait_send()


def summed_weight(latents, values_grad, n):
    rows, depth = latents.shape
    columns = values_grad.shape[1]
    width = depth // n
    vmem = pl.BlockSpec(memory_space=pltpu.VMEM)
    buffer = pltpu.VMEM((n // 2, width, columns), jnp.bfloat16)
    return pl.pallas_call(
        functools.partial(weight_kernel, "sp", n),
        out_shape=jax.ShapeDtypeStruct((width, columns), jnp.float32),
        in_specs=[vmem] * 2,
        out_specs=vmem,
        scratch_shapes=[buffer] * 4 + [pltpu.SemaphoreType.DMA((n // 2,))] * 4,
        compiler_params=pltpu.CompilerParams(collective_id=3, has_side_effects=True),
        cost_estimate=pl.CostEstimate(
            flops=2 * rows * depth * columns,
            bytes_accessed=depth * columns * 64,
            transcendentals=0,
        ),
    )(latents, values_grad)


def by_unit(
    queries,
    key_vectors,
    latents,
    value_weight,
    log_sums,
    out_first,
    out_second,
    cotangent,
    head_lambda,
):
    n = lax.axis_size("sp")
    rows = queries.shape[0]
    values = jnp.dot(latents, value_weight, preferred_element_type=jnp.float32).astype(jnp.bfloat16)
    packed, stats = send_units(
        queries, key_vectors, values, out_first, out_second, cotangent, log_sums.T, head_lambda, n
    )
    count = n * rows
    stats = stats.transpose(1, 0, 2).reshape(8, count // BLOCK, BLOCK).transpose(1, 0, 2)
    grads = attention(packed.reshape(count, 2 * DH + 2 * DV), stats, BLOCK)
    (grads,) = exchange([grads.reshape(n, rows, 2 * DH + DV)], "sp", n, 2)
    grad_queries, grad_keys, values_grad = unpack(grads, head_lambda)
    latent_partial = lax.dot_general(
        values_grad, value_weight, (((1,), (1,)), ((), ())), preferred_element_type=jnp.float32
    )
    grad_latents = lax.psum_scatter(
        latent_partial.astype(jnp.bfloat16), "tp", scatter_dimension=1, tiled=True
    )
    grad_weight = summed_weight(latents, values_grad, n)
    return (grad_queries, grad_keys, grad_latents, grad_weight)


def dispatch(queries, key_vectors, latents, value_weight, log_sums, *rest):
    n = lax.axis_size("sp")
    count = n * queries.shape[0]
    fits = rest[-1].shape[0] * 2 == n and count % BLOCK == 0
    fits = fits and latents.shape[1] % (n * DV) == 0
    run = by_unit if fits else per_device
    return run(queries, key_vectors, latents, value_weight, log_sums, *rest)


def solution(mesh):
    return jax.shard_map(
        dispatch,
        mesh=mesh,
        in_specs=(
            P("sp", "tp"),
            P("sp", "tp"),
            P("sp", None),
            P(None, "tp"),
            P("sp", "tp"),
            P("sp", "tp"),
            P("sp", "tp"),
            P("sp", "tp"),
            P("tp"),
        ),
        out_specs=(P("sp", "tp"), P("sp", "tp"), P("sp", "tp"), P("sp", "tp")),
        check_vma=False,
    )
```
